32 devices in a mesh: sp: 16 (over z, y, x), tp: 2 (over core).
Axes of the slice: x: 2, y: 2, z: 4, core: 2. Of those that a mesh axis runs over, the one named last changes fastest.
Arguments:
- block_input: bfloat16 [8192, 2048], P('sp'), may hold values from -6 to 6
- value_weight: bfloat16 [2048, 2048], P(None, 'tp'), may hold values from -0.125 to 0.125
- queries: bfloat16 [8192, 1024], P('sp', 'tp'), may hold values from -0.5 to 0.5
- key_rows: bfloat16 [8192, 1024], P('sp', 'tp'), may hold values from -0.5 to 0.5
- log_decay: float32 [8192, 32], P('sp', 'tp'), may hold values from -0.125 to 0, as said below
- out_grad: bfloat16 [8192, 2048], P('sp', 'tp'), may hold values from -6 to 6
Outputs:
- query_grad: float32 [8192, 1024], P('sp', 'tp')
- key_grad: float32 [8192, 1024], P('sp', 'tp')
- decay_grad: float32 [8192, 32], P('sp', 'tp')
- weight_grad: float32 [2048, 2048], P('sp', 'tp')
- row_norms: float32 [2048], P('sp')
The draws below stay inside these ranges and needn't reach their ends.
Inputs may be any that keep to these rules, and one draw needn't show every extreme that they name: `log_decay`: log decays of each position and head, never positive.
All inputs are finite; a program needn't handle non-finite values.
Results may differ from the reference program's by a relative error of at most 0.013.
Values sent between devices are 32-bit elements; how exact they have to be, the bound alone decides.
A program may use at most 128 MiB of HBM per device.

```python
import jax
import jax.numpy as jnp
from jax import lax

D = 2048
HEADS = 32
GROUPS = 8
HEAD_DIM = 64
STATE = 128
SPAN = 128
TOKENS = 8192


def draw_log_decay(key, part):
    pick_key, slow_key, fast_key, block_key, rough_key = jax.random.split(key, 5)
    fast_share = 0.5
    quick = jax.random.uniform(pick_key, (HEADS,)) < fast_share
    slow_rate = jax.random.uniform(slow_key, (HEADS,), minval=0.5, maxval=1.5) / TOKENS
    fast_rate = jax.random.uniform(fast_key, (HEADS,), minval=0.01, maxval=0.04)
    base_rate = jnp.where(quick, fast_rate, slow_rate)
    block_scale = jnp.exp(jax.random.uniform(block_key, (TOKENS // SPAN, HEADS), minval=-0.69, maxval=0.69))
    block_scale = jnp.repeat(block_scale, SPAN, axis=0)
    roughness = jax.random.uniform(rough_key, (TOKENS, HEADS), minval=0.5, maxval=1.5)
    return (-(base_rate[None, :] * block_scale * roughness)).astype(jnp.float32)


def levels(stream_key, dims, shards, low, largest):
    def one(position, parts):
        heights = jax.random.uniform(jax.random.fold_in(jax.random.fold_in(stream_key, 6), position), (parts,), jnp.float32, low / len(shards), largest / len(shards))
        return jnp.repeat(jnp.exp(heights), dims[position] // parts).reshape((-1,) + (1,) * (len(dims) - position - 1))

    loudness = one(*shards[0])
    for cut in shards[1:]:
        loudness = loudness * one(*cut)
    return loudness


def noise(own_key, shape, scale, limit, cuts=(), kind=jnp.bfloat16):
    level = levels(own_key, shape, cuts, -0.22, 0.18) if cuts else 1.0
    drawn = jax.random.normal(own_key, shape, jnp.float32) * scale * level
    return jnp.minimum(jnp.maximum(drawn, -limit), limit).astype(kind)


def setup_inputs(seed: int = 0) -> dict:
    arg_keys = jax.random.split(jax.random.key(seed), 7)
    block_input = noise(arg_keys[0], (TOKENS, D), 1.0, 6.0, ((0, 16),))
    value_weight = noise(arg_keys[1], (D, HEADS * HEAD_DIM), D ** -0.5, 0.125, ((1, 2),))
    queries = noise(arg_keys[2], (TOKENS, GROUPS * STATE), STATE ** -0.5, 0.5, ((0, 16), (1, 2)))
    key_rows = noise(arg_keys[3], (TOKENS, GROUPS * STATE), STATE ** -0.5, 0.5, ((0, 16), (1, 2)))
    log_decay = draw_log_decay(jax.random.fold_in(arg_keys[6], 71), 0)
    out_grad = noise(arg_keys[5], (TOKENS, HEADS * HEAD_DIM), 1.0, 6.0, ((0, 16), (1, 2)))
    return {"block_input": block_input, "value_weight": value_weight, "queries": queries, "key_rows": key_rows, "log_decay": log_decay, "out_grad": out_grad}


exact_mode = lax.Precision.HIGHEST

def block_step(memory, pieces):
    queries, key_rows, decays, values = pieces
    length = decays.shape[0]
    cumulative = jnp.cumsum(decays, axis=0)
    causal = (lax.iota(jnp.int32, length)[:, None] >= lax.iota(jnp.int32, length)[None, :])[:, :, None, None]
    log_gap = cumulative[:, None] - cumulative[None, :]
    weights = jnp.where(causal, jnp.exp(jnp.where(causal, log_gap, 0.0)), 0.0)
    scores = jnp.einsum('sgn,rgn->srg', queries, key_rows, precision=exact_mode)
    within = jnp.einsum('srgj,rgjp->sgjp', scores[..., None] * weights, values, precision=exact_mode)
    carried = jnp.einsum('sgn,gjpn->sgjp', queries, memory, precision=exact_mode) * jnp.exp(cumulative)[..., None]
    to_end = jnp.exp(cumulative[-1] - cumulative)
    fresh_state = jnp.einsum('rgn,rgjp->gjpn', key_rows, values * to_end[..., None], precision=exact_mode)
    new_memory = jnp.exp(cumulative[-1])[..., None, None] * memory + fresh_state
    return (new_memory, within + carried)

def reference(block_input, value_weight, queries, key_rows, log_decay, out_grad):
    values = jnp.dot(block_input, value_weight, preferred_element_type=jnp.float32).astype(jnp.bfloat16)
    total = queries.shape[0]
    groups = queries.shape[1] // STATE
    heads = log_decay.shape[1]
    per_group = heads // groups
    blocks = total // SPAN
    memory = jnp.zeros((groups, per_group, HEAD_DIM, STATE), jnp.float32)

    def forward(query_in, key_in, decay_in, value_in):
        pieces = (query_in.reshape(blocks, SPAN, groups, STATE), key_in.reshape(blocks, SPAN, groups, STATE), decay_in.reshape(blocks, SPAN, groups, per_group), value_in.reshape(blocks, SPAN, groups, per_group, HEAD_DIM))
        final, outputs = lax.scan(block_step, memory, pieces)
        return outputs.reshape(total, heads * HEAD_DIM)
    mixed, pullback = jax.vjp(forward, queries.astype(jnp.float32), key_rows.astype(jnp.float32), log_decay, values.astype(jnp.float32))
    query_grad, key_grad, decay_grad, value_grad = pullback(out_grad.astype(jnp.float32))
    rounded_grad = value_grad.astype(jnp.bfloat16)
    weight_grad = jnp.dot(block_input.T, rounded_grad, preferred_element_type=jnp.float32)
    row_norms = lax.optimization_barrier(jnp.sum(weight_grad * weight_grad, axis=1))
    return (query_grad, key_grad, decay_grad, weight_grad, row_norms)
```

```python
import functools

import jax
import jax.numpy as jnp
from jax import lax
from jax.experimental import pallas as pl
from jax.experimental.pallas import tpu as pltpu
from jax.sharding import PartitionSpec as P

HEAD_DIM = 64
STATE = 128
SPAN = 128
LANES = 128

F32 = jnp.float32
BF16 = jnp.bfloat16
HI = lax.Precision.HIGHEST
VMEM = pltpu.VMEM
MESH = pl.DeviceIdType.MESH
GRANT = 60 * 1024 * 1024


def dot(a, b, ca, cb, precision=None):
    return lax.dot_general(
        a, b, (((ca,), (cb,)), ((), ())), precision=precision, preferred_element_type=F32
    )


def square(size, test):
    rows = lax.broadcasted_iota(jnp.int32, (size, size), 0)
    cols = lax.broadcasted_iota(jnp.int32, (size, size), 1)
    return test(rows, cols)


def spread(columns, width):
    length, heads = columns.shape
    lane = lax.broadcasted_iota(jnp.int32, (length, width), 1)
    out = jnp.broadcast_to(columns[:, 0:1], (length, width))
    for j in range(1, heads):
        out = jnp.where(lane >= j * HEAD_DIM, columns[:, j : j + 1], out)
    return out


def own_kernel(x, w, q, k, ld, g, values, fresh, back, logs):
    rows = x.shape[0]
    heads = ld.shape[1]
    width = heads * HEAD_DIM
    tri = square(SPAN, lambda r, c: r >= c).astype(F32)
    v = dot(x[...], w[...], 1, 0).astype(BF16)
    values[...] = v
    pieces = []
    total = jnp.zeros((1, heads), F32)
    for c in range(rows // SPAN):
        cum = dot(tri, ld[0, :, c * SPAN : (c + 1) * SPAN], 1, 1, HI) + total
        total = cum[SPAN - 1 : SPAN, :]
        pieces.append(cum)
    state = jnp.zeros((width, STATE), F32)
    grad = jnp.zeros((width, STATE), F32)
    for c in range(rows // SPAN):
        at = slice(c * SPAN, (c + 1) * SPAN)
        to_end = spread(jnp.exp(total - pieces[c]), width)
        ve = (v[at, :].astype(F32) * to_end).astype(BF16)
        ge = (g[at, :].astype(F32) * spread(jnp.exp(pieces[c]), width)).astype(BF16)
        state = state + dot(ve, k[at, :], 0, 0)
        grad = grad + dot(ge, q[at, :], 0, 0)
    fresh[...] = state
    back[...] = grad
    for j in range(heads):
        logs[j] = jnp.broadcast_to(total[:, j : j + 1], logs.shape[1:])


def scan_kernel(n, chunk, fresh, back, logs, before, after,
                got_f, got_b, got_l, send_f, send_b, sems_out, sems_in, sems_out2, sems_in2):
    me = lax.axis_index("sp")
    per_head = HEAD_DIM // chunk

    barrier = pltpu.get_barrier_semaphore()

    def greet(d, _):
        pl.semaphore_signal(barrier, inc=1, device_id={"sp": lax.rem(me + d, n)}, device_id_type=MESH)
        return 0

    lax.fori_loop(1, n, greet, 0)
    pl.semaphore_wait(barrier, n - 1)

    def first(d):
        to = lax.rem(me + d, n)
        return [
            pltpu.make_async_remote_copy(
                src, dst, sems_out.at[kind, d], sems_in.at[kind, d],
                device_id={"sp": to}, device_id_type=MESH,
            )
            for kind, (src, dst) in enumerate((
                (fresh.at[to], got_f.at[me]),
                (back.at[to], got_b.at[me]),
                (logs.at[to // per_head], got_l.at[me]),
            ))
        ]

    def go(make):
        def body(d, _):
            for copy in make(d):
                copy.start()
            return 0
        lax.fori_loop(1, n, body, 0)

    def done(make):
        def body(d, _):
            for copy in make(d):
                copy.wait()
            return 0
        lax.fori_loop(1, n, body, 0)

    go(first)
    got_f[me] = fresh[me]
    got_b[me] = back[me]
    got_l[me] = logs[me // per_head]
    done(first)

    def forward(j, run):
        send_f[j] = run
        return jnp.exp(got_l[j][0:1, :]) * run + got_f[j]

    def backward(i, run):
        j = n - 1 - i
        send_b[j] = run
        return jnp.exp(got_l[j][0:1, :]) * run + got_b[j]

    zero = jnp.zeros((chunk, STATE), F32)
    lax.fori_loop(0, n, forward, zero)
    lax.fori_loop(0, n, backward, zero)

    def second(d):
        to = lax.rem(me + d, n)
        return [
            pltpu.make_async_remote_copy(
                src, dst, sems_out2.at[kind, d], sems_in2.at[kind, d],
                device_id={"sp": to}, device_id_type=MESH,
            )
            for kind, (src, dst) in enumerate((
                (send_b.at[to], after.at[me]),
                (send_f.at[to], before.at[me]),
            ))
        ]

    go(second)
    before[me] = send_f[me]
    after[me] = send_b[me]
    done(second)


def grad_kernel(q, k, v, g, ld, first_state, last_grad, dq, dk, dv, dd, states):
    rows = q.shape[0]
    heads = ld.shape[1]
    width = heads * HEAD_DIM
    blocks = rows // SPAN
    causal = square(SPAN, lambda r, c: r >= c)
    tri = causal.astype(F32)
    strict = square(SPAN, lambda r, c: r < c).astype(F32)
    lane = lax.broadcasted_iota(jnp.int32, (heads, width), 1)
    pick = ((lane >= HEAD_DIM * lax.broadcasted_iota(jnp.int32, (heads, width), 0))
            & (lane < HEAD_DIM * (1 + lax.broadcasted_iota(jnp.int32, (heads, width), 0)))).astype(F32)

    def sums(c):
        part = ld[0, :, c * SPAN : (c + 1) * SPAN]
        return dot(tri, part, 1, 1, HI), dot(part, tri, 1, 1, HI)

    def shrink(row, state):
        return jnp.concatenate(
            [jnp.exp(row[j : j + 1, SPAN - 1 : SPAN]) * state[j * HEAD_DIM : (j + 1) * HEAD_DIM]
             for j in range(heads)], axis=0)

    cums = [sums(c) for c in range(blocks)]
    states[0] = first_state[...]
    for c in range(blocks - 1):
        at = slice(c * SPAN, (c + 1) * SPAN)
        col, row = cums[c]
        to_end = spread(jnp.exp(col[SPAN - 1 : SPAN, :] - col), width)
        ve = (v[at, :].astype(F32) * to_end).astype(BF16)
        states[c + 1] = shrink(row, states[c]) + dot(ve, k[at, :], 0, 0)
    d_state = last_grad[...]
    for c in reversed(range(blocks)):
        at = slice(c * SPAN, (c + 1) * SPAN)
        col, row = cums[c]
        qc, kc = q[at, :], k[at, :]
        vc, gc = v[at, :], g[at, :]
        state = states[c]
        sb, db = state.astype(BF16), d_state.astype(BF16)
        to_end = spread(jnp.exp(col[SPAN - 1 : SPAN, :] - col), width)
        ge32 = gc.astype(F32) * spread(jnp.exp(col), width)
        v32 = vc.astype(F32)
        ge = ge32.astype(BF16)
        ve = (v32 * to_end).astype(BF16)
        y = dot(qc, sb, 1, 1)
        z = dot(kc, db, 1, 1) * to_end
        r_cross = dot(pick, ge32 * y, 1, 1, HI)
        c_cross = dot(pick, v32 * z, 1, 1, HI)
        scores = dot(qc, kc, 1, 1)
        d_scores = jnp.zeros((SPAN, SPAN), F32)
        r_in, c_in, d_values, through = [], [], [], []
        kept = shrink(row, state)
        for j in range(heads):
            head = slice(j * HEAD_DIM, (j + 1) * HEAD_DIM)
            gap = jnp.minimum(col[:, j : j + 1] - row[j : j + 1, :], 0.0)
            weight = jnp.where(causal, jnp.exp(gap), 0.0)
            t1 = dot(gc[:, head], vc[:, head], 1, 1) * weight
            d_scores = d_scores + t1
            pairs = t1 * scores
            r_in.append(jnp.sum(pairs, axis=1, keepdims=True))
            c_in.append(jnp.sum(pairs, axis=0, keepdims=True))
            d_values.append(dot((scores * weight).astype(BF16), gc[:, head], 0, 0))
            through.append(jnp.sum(kept[head, :] * d_state[head, :], keepdims=True))
        dv[at, :] = (jnp.concatenate(d_values, axis=1) + z).astype(BF16)
        dsb = d_scores.astype(BF16)
        dq[at, :] = dot(dsb, kc, 1, 0) + dot(ge, sb, 1, 0)
        dk[at, :] = dot(dsb, qc, 0, 0) + dot(ve, db, 1, 0)
        r_rows = dot(jnp.concatenate(r_in, axis=1), tri, 0, 0, HI)
        rest = dot(r_cross - jnp.concatenate(c_in, axis=0), tri, 1, 0, HI)
        dd[0, :, at] = (r_rows + rest + dot(c_cross, strict, 1, 0, HI)
                        + jnp.concatenate(through, axis=0))
        d_state = shrink(row, d_state) + dot(ge, qc, 0, 0)


def bits_of(n):
    return n.bit_length() - 1


def order_of(stream, bits):
    lead = min(3, bits)
    turn = stream % lead if lead else 0
    return [(turn + i) % lead for i in range(lead)] + list(range(lead, bits))


def weight_kernel(n, xt, dv, out, part, *rest):
    bits = bits_of(n)
    levels, (send, recv) = rest[:bits], rest[bits:]
    streams = part.shape[0]
    me = lax.axis_index("sp")
    mine = [lax.rem(me // (1 << b), 2) for b in range(bits)]
    partner = [me + (1 << b) * (1 - 2 * mine[b]) for b in range(bits)]

    barrier = pltpu.get_barrier_semaphore()
    for b in range(bits):
        pl.semaphore_signal(barrier, inc=1, device_id={"sp": partner[b]}, device_id_type=MESH)
    pl.semaphore_wait(barrier, bits)

    def fill(s, spots):
        order = order_of(s, bits)
        cols = dv[:, s * LANES : (s + 1) * LANES]
        for spot in spots:
            block = 0
            for place, b in enumerate(order):
                flip = (spot >> (bits - 1 - place)) & 1
                block = block + (1 << b) * ((1 - mine[b]) if flip else mine[b])
            part[s, spot] = dot(xt[block], cols, 1, 0)

    def hop(s, step):
        src = part if step == 0 else levels[step - 1]
        half = n >> (step + 1)
        return pltpu.make_async_remote_copy(
            src.at[s, pl.ds(half, half)], levels[step].at[s],
            send.at[s, step], recv.at[s, step],
            device_id={"sp": partner[order_of(s, bits)[step]]}, device_id_type=MESH,
        )

    for s in range(streams):
        fill(s, range(n // 2, n))
        hop(s, 0).start()
    for s in range(streams):
        fill(s, range(n // 2))
    for step in range(bits):
        half = n >> (step + 1)
        src = part if step == 0 else levels[step - 1]
        for s in range(streams):
            hop(s, step).wait_recv()
            if step == bits - 1:
                out[:, s * LANES : (s + 1) * LANES] = src[s, 0] + levels[step][s, 0]
            else:
                levels[step][s] = levels[step][s] + src[s, 0:half]
                hop(s, step + 1).start()
    for step in range(bits):
        for s in range(streams):
            hop(s, step).wait_send()


def on_device(n, block_input, value_weight, queries, key_rows, log_decay, out_grad):
    rows, model = block_input.shape
    heads = log_decay.shape[1]
    groups = queries.shape[1] // STATE
    per_group = heads // groups
    width = per_group * HEAD_DIM
    chunk = heads * HEAD_DIM // n
    blocks = rows // SPAN
    decays = log_decay.T.reshape(groups, per_group, rows)
    xt = block_input.T.reshape(n, model // n, rows)

    def by_group(cols):
        return pl.BlockSpec((rows, cols), lambda i: (0, i))

    ld_spec = pl.BlockSpec((1, per_group, rows), lambda i: (i, 0, 0))
    state_spec = pl.BlockSpec((width, STATE), lambda i: (i, 0))
    state_shape = jax.ShapeDtypeStruct((heads * HEAD_DIM, STATE), F32)
    values, fresh, back, logs = pl.pallas_call(
        own_kernel,
        grid=(groups,),
        in_specs=[
            pl.BlockSpec((rows, model), lambda i: (0, 0)),
            pl.BlockSpec((model, width), lambda i: (0, i)),
            by_group(STATE), by_group(STATE), ld_spec, by_group(width),
        ],
        out_specs=[
            by_group(width), state_spec, state_spec,
            pl.BlockSpec((per_group, 8, LANES), lambda i: (i, 0, 0)),
        ],
        out_shape=[
            jax.ShapeDtypeStruct((rows, heads * HEAD_DIM), BF16), state_shape, state_shape,
            jax.ShapeDtypeStruct((heads, 8, LANES), F32),
        ],
        compiler_params=pltpu.CompilerParams(vmem_limit_bytes=GRANT),
        name="own_states",
    )(block_input, value_weight, queries, key_rows, decays, out_grad)

    vm = pl.BlockSpec(memory_space=VMEM)
    piece = (n, chunk, STATE)
    before, after = pl.pallas_call(
        functools.partial(scan_kernel, n, chunk),
        in_specs=[vm] * 3,
        out_specs=[vm] * 2,
        out_shape=[jax.ShapeDtypeStruct(piece, F32)] * 2,
        scratch_shapes=[VMEM(piece, F32)] * 2 + [VMEM((n, 8, LANES), F32)] + [VMEM(piece, F32)] * 2
        + [pltpu.SemaphoreType.DMA((3, n))] * 2 + [pltpu.SemaphoreType.DMA((2, n))] * 2,
        compiler_params=pltpu.CompilerParams(collective_id=0, has_side_effects=True, vmem_limit_bytes=GRANT),
        name="scan_states",
    )(fresh.reshape(piece), back.reshape(piece), logs)

    query_grad, key_grad, rounded_grad, decay_rows = pl.pallas_call(
        grad_kernel,
        grid=(groups,),
        in_specs=[by_group(STATE), by_group(STATE), by_group(width), by_group(width), ld_spec,
                  state_spec, state_spec],
        out_specs=[by_group(STATE), by_group(STATE), by_group(width), ld_spec],
        out_shape=[
            jax.ShapeDtypeStruct(queries.shape, F32), jax.ShapeDtypeStruct(queries.shape, F32),
            jax.ShapeDtypeStruct((rows, heads * HEAD_DIM), BF16),
            jax.ShapeDtypeStruct((groups, per_group, rows), F32),
        ],
        scratch_shapes=[VMEM((blocks, width, STATE), F32)],
        compiler_params=pltpu.CompilerParams(vmem_limit_bytes=GRANT),
        name="mixer_grads",
    )(queries, key_rows, values, out_grad, decays,
      before.reshape(heads * HEAD_DIM, STATE), after.reshape(heads * HEAD_DIM, STATE))

    own_rows, columns = model // n, heads * HEAD_DIM
    streams = columns // LANES
    bits = bits_of(n)
    weight_grad = pl.pallas_call(
        functools.partial(weight_kernel, n),
        in_specs=[vm] * 2,
        out_specs=vm,
        out_shape=jax.ShapeDtypeStruct((own_rows, columns), F32),
        scratch_shapes=[VMEM((streams, n, own_rows, LANES), F32)]
        + [VMEM((streams, n >> (b + 1), own_rows, LANES), F32) for b in range(bits)]
        + [pltpu.SemaphoreType.DMA((streams, bits))] * 2,
        compiler_params=pltpu.CompilerParams(collective_id=1, has_side_effects=True, vmem_limit_bytes=GRANT),
        name="weight_grad",
    )(xt, rounded_grad)
    row_norms = lax.psum(jnp.sum(weight_grad * weight_grad, axis=1), "tp")
    return query_grad, key_grad, decay_rows.reshape(heads, rows).T, weight_grad, row_norms


def solution(mesh):
    in_specs = (
        P("sp", None),
        P(None, "tp"),
        P("sp", "tp"),
        P("sp", "tp"),
        P("sp", "tp"),
        P("sp", "tp"),
    )
    out_specs = (P("sp", "tp"), P("sp", "tp"), P("sp", "tp"), P("sp", "tp"), P("sp"))
    return jax.shard_map(
        functools.partial(on_device, mesh.shape["sp"]),
        mesh=mesh, in_specs=in_specs, out_specs=out_specs, check_vma=False,
    )
```

```python
import functools

import jax
import jax.numpy as jnp
from jax import lax
from jax.experimental import pallas as pl
from jax.experimental.pallas import tpu as pltpu
from jax.sharding import PartitionSpec as P

HEAD_DIM = 64
STATE = 128
SPAN = 128
LANES = 128

F32 = jnp.float32
BF16 = jnp.bfloat16
HI = lax.Precision.HIGHEST
VMEM = pltpu.VMEM
MESH = pl.DeviceIdType.MESH
GRANT = 60 * 1024 * 1024


def dot(a, b, ca, cb, precision=None):
    return lax.dot_general(
        a, b, (((ca,), (cb,)), ((), ())), precision=precision, preferred_element_type=F32
    )


def square(size, test):
    rows = lax.broadcasted_iota(jnp.int32, (size, size), 0)
    cols = lax.broadcasted_iota(jnp.int32, (size, size), 1)
    return test(rows, cols)


def spread(columns, width):
    length, heads = columns.shape
    lane = lax.broadcasted_iota(jnp.int32, (length, width), 1)
    out = jnp.broadcast_to(columns[:, 0:1], (length, width))
    for j in range(1, heads):
        out = jnp.where(lane >= j * HEAD_DIM, columns[:, j : j + 1], out)
    return out


def own_kernel(x, w, q, k, ld, g, values, fresh, back, logs):
    rows = x.shape[0]
    heads = ld.shape[1]
    width = heads * HEAD_DIM
    tri = square(SPAN, lambda r, c: r >= c).astype(F32)
    v = dot(x[...], w[...], 1, 0).astype(BF16)
    values[...] = v
    pieces = []
    total = jnp.zeros((1, heads), F32)
    for c in range(rows // SPAN):
        cum = dot(tri, ld[0, :, c * SPAN : (c + 1) * SPAN], 1, 1, HI) + total
        total = cum[SPAN - 1 : SPAN, :]
        pieces.append(cum)
    state = jnp.zeros((width, STATE), F32)
    grad = jnp.zeros((width, STATE), F32)
    for c in range(rows // SPAN):
        at = slice(c * SPAN, (c + 1) * SPAN)
        to_end = spread(jnp.exp(total - pieces[c]), width)
        ve = (v[at, :].astype(F32) * to_end).astype(BF16)
        ge = (g[at, :].astype(F32) * spread(jnp.exp(pieces[c]), width)).astype(BF16)
        state = state + dot(ve, k[at, :], 0, 0)
        grad = grad + dot(ge, q[at, :], 0, 0)
    fresh[...] = state
    back[...] = grad
    for j in range(heads):
        logs[j] = jnp.broadcast_to(total[:, j : j + 1], logs.shape[1:])


def scan_kernel(n, chunk, fresh, back, logs, before, after,
                got_f, got_b, got_l, send_f, send_b, sems_out, sems_in, sems_out2, sems_in2):
    me = lax.axis_index("sp")
    per_head = HEAD_DIM // chunk

    barrier = pltpu.get_barrier_semaphore()

    def greet(d, _):
        pl.semaphore_signal(barrier, inc=1, device_id={"sp": lax.rem(me + d, n)}, device_id_type=MESH)
        return 0

    lax.fori_loop(1, n, greet, 0)
    pl.semaphore_wait(barrier, n - 1)

    def first(d):
        to = lax.rem(me + d, n)
        return [
            pltpu.make_async_remote_copy(
                src, dst, sems_out.at[kind, d], sems_in.at[kind, d],
                device_id={"sp": to}, device_id_type=MESH,
            )
            for kind, (src, dst) in enumerate((
                (fresh.at[to], got_f.at[me]),
                (back.at[to], got_b.at[me]),
                (logs.at[to // per_head], got_l.at[me]),
            ))
        ]

    def go(make):
        def body(d, _):
            for copy in make(d):
                copy.start()
            return 0
        lax.fori_loop(1, n, body, 0)

    def done(make):
        def body(d, _):
            for copy in make(d):
                copy.wait()
            return 0
        lax.fori_loop(1, n, body, 0)

    go(first)
    got_f[me] = fresh[me]
    got_b[me] = back[me]
    got_l[me] = logs[me // per_head]
    done(first)

    def forward(j, run):
        send_f[j] = run
        return jnp.exp(got_l[j][0:1, :]) * run + got_f[j]

    def backward(i, run):
        j = n - 1 - i
        send_b[j] = run
        return jnp.exp(got_l[j][0:1, :]) * run + got_b[j]

    zero = jnp.zeros((chunk, STATE), F32)
    lax.fori_loop(0, n, forward, zero)
    lax.fori_loop(0, n, backward, zero)

    def second(d):
        to = lax.rem(me + d, n)
        return [
            pltpu.make_async_remote_copy(
                src, dst, sems_out2.at[kind, d], sems_in2.at[kind, d],
                device_id={"sp": to}, device_id_type=MESH,
            )
            for kind, (src, dst) in enumerate((
                (send_b.at[to], after.at[me]),
                (send_f.at[to], before.at[me]),
            ))
        ]

    go(second)
    before[me] = send_f[me]
    after[me] = send_b[me]
    done(second)


def loop_blocks(q, k, v, g, ld, i):
    heads = ld.shape[1]
    width = heads * HEAD_DIM
    causal = square(SPAN, lambda r, c: r >= c)
    tri = causal.astype(F32)

    def read(c):
        at = pl.ds(pl.multiple_of(c * SPAN, SPAN), SPAN)
        part = ld[i, :, at]
        col, row = dot(tri, part, 1, 1, HI), dot(part, tri, 1, 1, HI)
        lanes = slice(i * STATE, (i + 1) * STATE)
        wide = slice(i * width, (i + 1) * width)
        to_end = spread(jnp.exp(col[SPAN - 1 : SPAN, :] - col), width)
        grown = spread(jnp.exp(col), width)
        return at, col, row, q[at, lanes], k[at, lanes], v[at, wide], g[at, wide], to_end, grown

    def weight(col, row, j):
        gap = jnp.minimum(col[:, j : j + 1] - row[j : j + 1, :], 0.0)
        return jnp.where(causal, jnp.exp(gap), 0.0)

    return heads, width, tri, read, weight


def shrink(row, state):
    return jnp.concatenate(
        [jnp.exp(row[j : j + 1, SPAN - 1 : SPAN]) * state[j * HEAD_DIM : (j + 1) * HEAD_DIM]
         for j in range(row.shape[0])], axis=0)


def value_pass(refs, i, last_grad, dv, grads):
    q, k, v, g, ld = refs
    heads, width, tri, read, weight = loop_blocks(q, k, v, g, ld, i)
    blocks = q.shape[0] // SPAN

    def one(step, d_state):
        c = blocks - 1 - step
        at, col, row, qc, kc, vc, gc, to_end, grown = read(c)
        grads[i, c] = d_state
        z = dot(kc, d_state.astype(BF16), 1, 1) * to_end
        scores = dot(qc, kc, 1, 1)
        parts = [
            dot((scores * weight(col, row, j)).astype(BF16),
                gc[:, j * HEAD_DIM : (j + 1) * HEAD_DIM], 0, 0)
            for j in range(heads)
        ]
        dv[at, i * width : (i + 1) * width] = (jnp.concatenate(parts, axis=1) + z).astype(BF16)
        ge = (gc.astype(F32) * grown).astype(BF16)
        return shrink(row, d_state) + dot(ge, qc, 0, 0)

    lax.fori_loop(0, blocks, one, last_grad[i * width : (i + 1) * width, :])


def rest_pass(refs, i, first_state, grads, dq, dk, dd):
    q, k, v, g, ld = refs
    heads, width, tri, read, weight = loop_blocks(q, k, v, g, ld, i)
    blocks = q.shape[0] // SPAN
    strict = square(SPAN, lambda r, c: r < c).astype(F32)
    lane = lax.broadcasted_iota(jnp.int32, (heads, width), 1)
    low = HEAD_DIM * lax.broadcasted_iota(jnp.int32, (heads, width), 0)
    pick = ((lane >= low) & (lane < low + HEAD_DIM)).astype(F32)
    lanes = slice(i * STATE, (i + 1) * STATE)

    def one(c, state):
        at, col, row, qc, kc, vc, gc, to_end, grown = read(c)
        d_state = grads[i, c]
        sb, db = state.astype(BF16), d_state.astype(BF16)
        ge32 = gc.astype(F32) * grown
        v32 = vc.astype(F32)
        ge = ge32.astype(BF16)
        ve = (v32 * to_end).astype(BF16)
        r_cross = dot(pick, ge32 * dot(qc, sb, 1, 1), 1, 1, HI)
        c_cross = dot(pick, v32 * (dot(kc, db, 1, 1) * to_end), 1, 1, HI)
        scores = dot(qc, kc, 1, 1)
        d_scores = jnp.zeros((SPAN, SPAN), F32)
        r_in, c_in, through = [], [], []
        kept = shrink(row, state)
        for j in range(heads):
            head = slice(j * HEAD_DIM, (j + 1) * HEAD_DIM)
            t1 = dot(gc[:, head], vc[:, head], 1, 1) * weight(col, row, j)
            d_scores = d_scores + t1
            pairs = t1 * scores
            r_in.append(jnp.sum(pairs, axis=1, keepdims=True))
            c_in.append(jnp.sum(pairs, axis=0, keepdims=True))
            through.append(jnp.sum(kept[head, :] * d_state[head, :], keepdims=True))
        dsb = d_scores.astype(BF16)
        dq[at, lanes] = dot(dsb, kc, 1, 0) + dot(ge, sb, 1, 0)
        dk[at, lanes] = dot(dsb, qc, 0, 0) + dot(ve, db, 1, 0)
        r_rows = dot(jnp.concatenate(r_in, axis=1), tri, 0, 0, HI)
        rest = dot(r_cross - jnp.concatenate(c_in, axis=0), tri, 1, 0, HI)
        dd[i, :, at] = (r_rows + rest + dot(c_cross, strict, 1, 0, HI)
                        + jnp.concatenate(through, axis=0))
        return kept + dot(ve, kc, 0, 0)

    lax.fori_loop(0, blocks, one, first_state[i * width : (i + 1) * width, :])


def bits_of(n):
    return n.bit_length() - 1


def order_of(stream, bits):
    lead = min(3, bits)
    turn = stream % lead if lead else 0
    return [(turn + i) % lead for i in range(lead)] + list(range(lead, bits))


def weight_kernel(n, tp, xt, q, k, v, g, ld, first_state, last_grad, dq, dk, dd, out, norms,
                  part, dv, grads, own_norm, got_norm, *rest):
    bits = bits_of(n)
    levels, (send, recv, send_n, recv_n) = rest[:bits], rest[bits:]
    streams = part.shape[0]
    groups = ld.shape[0]
    per_stream = ld.shape[1] * HEAD_DIM // LANES
    refs = (q, k, v, g, ld)
    me = lax.axis_index("sp")
    side = lax.axis_index("tp")
    mine = [lax.rem(me // (1 << b), 2) for b in range(bits)]
    partner = [me + (1 << b) * (1 - 2 * mine[b]) for b in range(bits)]

    barrier = pltpu.get_barrier_semaphore()
    for b in range(bits):
        pl.semaphore_signal(barrier, inc=1, device_id={"sp": partner[b]}, device_id_type=MESH)
    for d in range(1, tp):
        pl.semaphore_signal(barrier, inc=1, device_id={"tp": lax.rem(side + d, tp)}, device_id_type=MESH)
    pl.semaphore_wait(barrier, bits + tp - 1)

    def fill(s, spots):
        order = order_of(s, bits)
        cols = dv[:, s * LANES : (s + 1) * LANES]
        for spot in spots:
            block = 0
            for place, b in enumerate(order):
                flip = (spot >> (bits - 1 - place)) & 1
                block = block + (1 << b) * ((1 - mine[b]) if flip else mine[b])
            part[s, spot] = dot(xt[block], cols, 1, 0)

    def hop(s, step):
        src = part if step == 0 else levels[step - 1]
        half = n >> (step + 1)
        return pltpu.make_async_remote_copy(
            src.at[s, pl.ds(half, half)], levels[step].at[s],
            send.at[s, step], recv.at[s, step],
            device_id={"sp": partner[order_of(s, bits)[step]]}, device_id_type=MESH,
        )

    def advance(team, step):
        half = n >> (step + 1)
        src = part if step == 0 else levels[step - 1]
        for s in team:
            hop(s, step).wait_recv()
            if step == bits - 1:
                out[:, s * LANES : (s + 1) * LANES] = src[s, 0] + levels[step][s, 0]
            else:
                levels[step][s] = levels[step][s] + src[s, 0:half]
                hop(s, step + 1).start()

    teams = [range(s, min(s + 3, streams)) for s in range(0, streams, 3)]
    to_do = list(range(groups))
    ready = 0
    at_step = {}

    def one_rest():
        if to_do:
            rest_pass(refs, to_do.pop(0), first_state, grads, dq, dk, dd)

    def push():
        for t in list(at_step):
            advance(teams[t], at_step[t])
            at_step[t] += 1
            if at_step[t] == bits:
                del at_step[t]

    for t, team in enumerate(teams):
        for s in team:
            while ready <= s // per_stream:
                value_pass(refs, ready, last_grad, dv, grads)
                ready += 1
            fill(s, range(n // 2, n))
            hop(s, 0).start()
        for s in team:
            fill(s, range(n // 2))
        push()
        at_step[t] = 0
    while at_step:
        one_rest()
        push()
    while to_do:
        one_rest()
    total = jnp.sum(out[...] * out[...], axis=1, keepdims=True)
    own_norm[...] = jnp.broadcast_to(total, own_norm.shape)

    def give(d):
        return pltpu.make_async_remote_copy(
            own_norm, got_norm.at[d], send_n.at[d], recv_n.at[d],
            device_id={"tp": lax.rem(side + d, tp)}, device_id_type=MESH,
        )

    for d in range(1, tp):
        give(d).start()
    for step in range(bits):
        for s in range(streams):
            hop(s, step).wait_send()
    for d in range(1, tp):
        give(d).wait()
    full = own_norm[...]
    for d in range(1, tp):
        full = full + got_norm[d]
    norms[...] = full


def on_device(n, tp, block_input, value_weight, queries, key_rows, log_decay, out_grad):
    rows, model = block_input.shape
    heads = log_decay.shape[1]
    groups = queries.shape[1] // STATE
    per_group = heads // groups
    width = per_group * HEAD_DIM
    chunk = heads * HEAD_DIM // n
    blocks = rows // SPAN
    decays = log_decay.T.reshape(groups, per_group, rows)
    xt = block_input.T.reshape(n, model // n, rows)

    def by_group(cols):
        return pl.BlockSpec((rows, cols), lambda i: (0, i))

    ld_spec = pl.BlockSpec((1, per_group, rows), lambda i: (i, 0, 0))
    state_spec = pl.BlockSpec((width, STATE), lambda i: (i, 0))
    state_shape = jax.ShapeDtypeStruct((heads * HEAD_DIM, STATE), F32)
    values, fresh, back, logs = pl.pallas_call(
        own_kernel,
        grid=(groups,),
        in_specs=[
            pl.BlockSpec((rows, model), lambda i: (0, 0)),
            pl.BlockSpec((model, width), lambda i: (0, i)),
            by_group(STATE), by_group(STATE), ld_spec, by_group(width),
        ],
        out_specs=[
            by_group(width), state_spec, state_spec,
            pl.BlockSpec((per_group, 8, LANES), lambda i: (i, 0, 0)),
        ],
        out_shape=[
            jax.ShapeDtypeStruct((rows, heads * HEAD_DIM), BF16), state_shape, state_shape,
            jax.ShapeDtypeStruct((heads, 8, LANES), F32),
        ],
        compiler_params=pltpu.CompilerParams(vmem_limit_bytes=GRANT),
        name="own_states",
    )(block_input, value_weight, queries, key_rows, decays, out_grad)

    vm = pl.BlockSpec(memory_space=VMEM)
    piece = (n, chunk, STATE)
    before, after = pl.pallas_call(
        functools.partial(scan_kernel, n, chunk),
        in_specs=[vm] * 3,
        out_specs=[vm] * 2,
        out_shape=[jax.ShapeDtypeStruct(piece, F32)] * 2,
        scratch_shapes=[VMEM(piece, F32)] * 2 + [VMEM((n, 8, LANES), F32)] + [VMEM(piece, F32)] * 2
        + [pltpu.SemaphoreType.DMA((3, n))] * 2 + [pltpu.SemaphoreType.DMA((2, n))] * 2,
        compiler_params=pltpu.CompilerParams(collective_id=0, has_side_effects=True, vmem_limit_bytes=GRANT),
        name="scan_states",
    )(fresh.reshape(piece), back.reshape(piece), logs)

    own_rows, columns = model // n, heads * HEAD_DIM
    streams = columns // LANES
    bits = bits_of(n)
    query_grad, key_grad, decay_rows, weight_grad, norms = pl.pallas_call(
        functools.partial(weight_kernel, n, tp),
        in_specs=[vm] * 8,
        out_specs=[vm] * 5,
        out_shape=[
            jax.ShapeDtypeStruct(queries.shape, F32), jax.ShapeDtypeStruct(queries.shape, F32),
            jax.ShapeDtypeStruct((groups, per_group, rows), F32),
            jax.ShapeDtypeStruct((own_rows, columns), F32),
            jax.ShapeDtypeStruct((own_rows, LANES), F32),
        ],
        scratch_shapes=[
            VMEM((streams, n, own_rows, LANES), F32), VMEM((rows, columns), BF16),
            VMEM((groups, blocks, width, STATE), F32),
            VMEM((own_rows, LANES), F32), VMEM((tp, own_rows, LANES), F32),
        ]
        + [VMEM((streams, n >> (b + 1), own_rows, LANES), F32) for b in range(bits)]
        + [pltpu.SemaphoreType.DMA((streams, bits))] * 2 + [pltpu.SemaphoreType.DMA((tp,))] * 2,
        compiler_params=pltpu.CompilerParams(collective_id=1, has_side_effects=True, vmem_limit_bytes=GRANT),
        name="weight_grad",
    )(xt, queries, key_rows, values, out_grad, decays,
      before.reshape(heads * HEAD_DIM, STATE), after.reshape(heads * HEAD_DIM, STATE))
    return query_grad, key_grad, decay_rows.reshape(heads, rows).T, weight_grad, norms[:, 0]


def solution(mesh):
    in_specs = (
        P("sp", None),
        P(None, "tp"),
        P("sp", "tp"),
        P("sp", "tp"),
        P("sp", "tp"),
        P("sp", "tp"),
    )
    out_specs = (P("sp", "tp"), P("sp", "tp"), P("sp", "tp"), P("sp", "tp"), P("sp"))
    return jax.shard_map(
        functools.partial(on_device, mesh.shape["sp"], mesh.shape["tp"]),
        mesh=mesh, in_specs=in_specs, out_specs=out_specs, check_vma=False,
    )
```

```python
import functools

import jax
import jax.numpy as jnp
from jax import lax
from jax.experimental import pallas as pl
from jax.experimental.pallas import tpu as pltpu
from jax.sharding import PartitionSpec as P

HEAD_DIM = 64
STATE = 128
SPAN = 128
LANES = 128

F32 = jnp.float32
BF16 = jnp.bfloat16
HI = lax.Precision.HIGHEST
VMEM = pltpu.VMEM
MESH = pl.DeviceIdType.MESH
GRANT = 60 * 1024 * 1024


def dot(a, b, ca, cb, precision=None):
    return lax.dot_general(
        a, b, (((ca,), (cb,)), ((), ())), precision=precision, preferred_element_type=F32
    )


def square(size, test):
    rows = lax.broadcasted_iota(jnp.int32, (size, size), 0)
    cols = lax.broadcasted_iota(jnp.int32, (size, size), 1)
    return test(rows, cols)


def spread(columns, width):
    length, heads = columns.shape
    lane = lax.broadcasted_iota(jnp.int32, (length, width), 1)
    out = jnp.broadcast_to(columns[:, 0:1], (length, width))
    for j in range(1, heads):
        out = jnp.where(lane >= j * HEAD_DIM, columns[:, j : j + 1], out)
    return out


def own_kernel(x, w, q, k, ld, g, values, fresh, back, logs):
    rows = x.shape[0]
    heads = ld.shape[1]
    width = heads * HEAD_DIM
    tri = square(SPAN, lambda r, c: r >= c).astype(F32)
    v = dot(x[...], w[...], 1, 0).astype(BF16)
    values[...] = v
    pieces = []
    total = jnp.zeros((1, heads), F32)
    for c in range(rows // SPAN):
        cum = dot(tri, ld[0, :, c * SPAN : (c + 1) * SPAN], 1, 1, HI) + total
        total = cum[SPAN - 1 : SPAN, :]
        pieces.append(cum)
    state = jnp.zeros((width, STATE), F32)
    grad = jnp.zeros((width, STATE), F32)
    for c in range(rows // SPAN):
        at = slice(c * SPAN, (c + 1) * SPAN)
        to_end = spread(jnp.exp(total - pieces[c]), width)
        ve = (v[at, :].astype(F32) * to_end).astype(BF16)
        ge = (g[at, :].astype(F32) * spread(jnp.exp(pieces[c]), width)).astype(BF16)
        state = state + dot(ve, k[at, :], 0, 0)
        grad = grad + dot(ge, q[at, :], 0, 0)
    fresh[...] = state
    back[...] = grad
    for j in range(heads):
        logs[j] = jnp.broadcast_to(total[:, j : j + 1], logs.shape[1:])


def scan_kernel(inner, outer, fresh, back, logs, before, after, got_f, got_b, got_l, send_f, send_b,
                total, total_l, far, far_l, *sems):
    me = lax.axis_index("sp")
    near, far_at = lax.rem(me, inner), me // inner
    per_log = inner * got_l.shape[1] // logs.shape[0]

    def near_peer(d):
        return far_at * inner + lax.rem(near + d, inner)

    def far_peer(d):
        return lax.rem(far_at + d, outer) * inner + near

    barrier = pltpu.get_barrier_semaphore()
    peers = [near_peer(d) for d in range(1, inner)] + [far_peer(d) for d in range(1, outer)]
    for to in peers:
        pl.semaphore_signal(barrier, inc=1, device_id={"sp": to}, device_id_type=MESH)
    pl.semaphore_wait(barrier, len(peers))

    def copies(pairs, out_sem, in_sem, d, to):
        return [
            pltpu.make_async_remote_copy(
                src, dst, out_sem.at[kind, d], in_sem.at[kind, d],
                device_id={"sp": to}, device_id_type=MESH,
            )
            for kind, (src, dst) in enumerate(pairs)
        ]

    def log_of(to):
        tall = got_l.shape[1]
        return pl.ds(to // per_log if tall == 1 else to * tall, tall)

    first, second, third = [], [], []
    for d in range(1, inner):
        to = lax.rem(near + d, inner)
        first += copies(((fresh.at[to], got_f.at[near]), (back.at[to], got_b.at[near]),
                         (logs.at[log_of(to)], got_l.at[near])), sems[0], sems[1], d, near_peer(d))
        third += copies(((send_b.at[to], after.at[near]), (send_f.at[to], before.at[near])),
                        sems[4], sems[5], d, near_peer(d))
    for d in range(1, outer):
        wrapped = (far_at + d) // outer
        second += copies(((total.at[wrapped], far.at[far_at]), (total_l, far_l.at[far_at])),
                         sems[2], sems[3], d, far_peer(d))

    for copy in first:
        copy.start()
    got_f[near] = fresh[near]
    got_b[near] = back[near]
    got_l[near] = logs[log_of(near)]
    for copy in first:
        copy.wait()

    def carry(log, run, new):
        return jnp.exp(log[:, 0:1, :]) * run + new

    ahead, behind = got_f[0], got_b[inner - 1]
    log = got_l[0]
    for c in range(1, inner):
        ahead = carry(got_l[c], ahead, got_f[c])
        behind = carry(got_l[inner - 1 - c], behind, got_b[inner - 1 - c])
        log = log + got_l[c]
    total[0] = ahead
    total[1] = behind
    total_l[...] = log
    for copy in second:
        copy.start()
    for copy in second:
        copy.wait()

    zero = jnp.zeros(ahead.shape, F32)
    run = lax.fori_loop(0, far_at, lambda j, r: carry(far_l[j], r, far[j]), zero)
    for c in range(inner):
        send_f[c] = run
        run = carry(got_l[c], run, got_f[c])
    run = lax.fori_loop(
        0, outer - 1 - far_at,
        lambda i, r: carry(far_l[outer - 1 - i], r, far[outer - 1 - i]), zero)
    for c in reversed(range(inner)):
        send_b[c] = run
        run = carry(got_l[c], run, got_b[c])
    for copy in third:
        copy.start()
    before[near] = send_f[near]
    after[near] = send_b[near]
    for copy in third:
        copy.wait()


def loop_blocks(q, k, v, g, ld, i):
    heads = ld.shape[1]
    width = heads * HEAD_DIM
    causal = square(SPAN, lambda r, c: r >= c)
    tri = causal.astype(F32)

    def read(c):
        at = pl.ds(pl.multiple_of(c * SPAN, SPAN), SPAN)
        part = ld[i, :, at]
        col, row = dot(tri, part, 1, 1, HI), dot(part, tri, 1, 1, HI)
        lanes = slice(i * STATE, (i + 1) * STATE)
        wide = slice(i * width, (i + 1) * width)
        to_end = spread(jnp.exp(col[SPAN - 1 : SPAN, :] - col), width)
        grown = spread(jnp.exp(col), width)
        return at, col, row, q[at, lanes], k[at, lanes], v[at, wide], g[at, wide], to_end, grown

    def weight(col, row, j):
        gap = jnp.minimum(col[:, j : j + 1] - row[j : j + 1, :], 0.0)
        return jnp.where(causal, jnp.exp(gap), 0.0)

    return heads, width, tri, read, weight


def shrink(row, state):
    return jnp.concatenate(
        [jnp.exp(row[j : j + 1, SPAN - 1 : SPAN]) * state[j * HEAD_DIM : (j + 1) * HEAD_DIM]
         for j in range(row.shape[0])], axis=0)


def value_pass(refs, i, last_grad, dv, grads):
    q, k, v, g, ld = refs
    heads, width, tri, read, weight = loop_blocks(q, k, v, g, ld, i)
    blocks = q.shape[0] // SPAN

    def one(step, d_state):
        c = blocks - 1 - step
        at, col, row, qc, kc, vc, gc, to_end, grown = read(c)
        grads[i, c] = d_state
        z = dot(kc, d_state.astype(BF16), 1, 1) * to_end
        scores = dot(qc, kc, 1, 1)
        parts = [
            dot((scores * weight(col, row, j)).astype(BF16),
                gc[:, j * HEAD_DIM : (j + 1) * HEAD_DIM], 0, 0)
            for j in range(heads)
        ]
        dv[at, i * width : (i + 1) * width] = (jnp.concatenate(parts, axis=1) + z).astype(BF16)
        ge = (gc.astype(F32) * grown).astype(BF16)
        return shrink(row, d_state) + dot(ge, qc, 0, 0)

    lax.fori_loop(0, blocks, one, last_grad[i * width : (i + 1) * width, :])


def rest_pass(refs, i, first_state, grads, dq, dk, dd):
    q, k, v, g, ld = refs
    heads, width, tri, read, weight = loop_blocks(q, k, v, g, ld, i)
    blocks = q.shape[0] // SPAN
    strict = square(SPAN, lambda r, c: r < c).astype(F32)
    lane = lax.broadcasted_iota(jnp.int32, (heads, width), 1)
    low = HEAD_DIM * lax.broadcasted_iota(jnp.int32, (heads, width), 0)
    pick = ((lane >= low) & (lane < low + HEAD_DIM)).astype(F32)
    lanes = slice(i * STATE, (i + 1) * STATE)

    def one(c, state):
        at, col, row, qc, kc, vc, gc, to_end, grown = read(c)
        d_state = grads[i, c]
        sb, db = state.astype(BF16), d_state.astype(BF16)
        ge32 = gc.astype(F32) * grown
        v32 = vc.astype(F32)
        ge = ge32.astype(BF16)
        ve = (v32 * to_end).astype(BF16)
        r_cross = dot(pick, ge32 * dot(qc, sb, 1, 1), 1, 1, HI)
        c_cross = dot(pick, v32 * (dot(kc, db, 1, 1) * to_end), 1, 1, HI)
        scores = dot(qc, kc, 1, 1)
        d_scores = jnp.zeros((SPAN, SPAN), F32)
        r_in, c_in, through = [], [], []
        kept = shrink(row, state)
        for j in range(heads):
            head = slice(j * HEAD_DIM, (j + 1) * HEAD_DIM)
            t1 = dot(gc[:, head], vc[:, head], 1, 1) * weight(col, row, j)
            d_scores = d_scores + t1
            pairs = t1 * scores
            r_in.append(jnp.sum(pairs, axis=1, keepdims=True))
            c_in.append(jnp.sum(pairs, axis=0, keepdims=True))
            through.append(jnp.sum(kept[head, :] * d_state[head, :], keepdims=True))
        dsb = d_scores.astype(BF16)
        dq[at, lanes] = dot(dsb, kc, 1, 0) + dot(ge, sb, 1, 0)
        dk[at, lanes] = dot(dsb, qc, 0, 0) + dot(ve, db, 1, 0)
        r_rows = dot(jnp.concatenate(r_in, axis=1), tri, 0, 0, HI)
        rest = dot(r_cross - jnp.concatenate(c_in, axis=0), tri, 1, 0, HI)
        dd[i, :, at] = (r_rows + rest + dot(c_cross, strict, 1, 0, HI)
                        + jnp.concatenate(through, axis=0))
        return kept + dot(ve, kc, 0, 0)

    lax.fori_loop(0, blocks, one, first_state[i * width : (i + 1) * width, :])


def bits_of(n):
    return n.bit_length() - 1


def order_of(stream, bits):
    lead = min(3, bits)
    turn = stream % lead if lead else 0
    return [(turn + i) % lead for i in range(lead)] + list(range(lead, bits))


def weight_kernel(n, tp, xt, q, k, v, g, ld, first_state, last_grad, dq, dk, dd, out, norms,
                  part, dv, grads, own_norm, got_norm, *rest):
    bits = bits_of(n)
    levels, (send, recv, send_n, recv_n) = rest[:bits], rest[bits:]
    streams = part.shape[0]
    groups = ld.shape[0]
    per_stream = ld.shape[1] * HEAD_DIM // LANES
    refs = (q, k, v, g, ld)
    me = lax.axis_index("sp")
    side = lax.axis_index("tp")
    mine = [lax.rem(me // (1 << b), 2) for b in range(bits)]
    partner = [me + (1 << b) * (1 - 2 * mine[b]) for b in range(bits)]

    barrier = pltpu.get_barrier_semaphore()
    for b in range(bits):
        pl.semaphore_signal(barrier, inc=1, device_id={"sp": partner[b]}, device_id_type=MESH)
    for d in range(1, tp):
        pl.semaphore_signal(barrier, inc=1, device_id={"tp": lax.rem(side + d, tp)}, device_id_type=MESH)
    pl.semaphore_wait(barrier, bits + tp - 1)

    def fill(s, spots):
        order = order_of(s, bits)
        cols = dv[:, s * LANES : (s + 1) * LANES]
        for spot in spots:
            block = 0
            for place, b in enumerate(order):
                flip = (spot >> (bits - 1 - place)) & 1
                block = block + (1 << b) * ((1 - mine[b]) if flip else mine[b])
            part[s, spot] = dot(xt[block], cols, 1, 0)

    def hop(s, step):
        src = part if step == 0 else levels[step - 1]
        half = n >> (step + 1)
        return pltpu.make_async_remote_copy(
            src.at[s, pl.ds(half, half)], levels[step].at[s],
            send.at[s, step], recv.at[s, step],
            device_id={"sp": partner[order_of(s, bits)[step]]}, device_id_type=MESH,
        )

    def advance(team, step):
        half = n >> (step + 1)
        src = part if step == 0 else levels[step - 1]
        for s in team:
            hop(s, step).wait_recv()
            if step == bits - 1:
                out[:, s * LANES : (s + 1) * LANES] = src[s, 0] + levels[step][s, 0]
            else:
                levels[step][s] = levels[step][s] + src[s, 0:half]
                hop(s, step + 1).start()

    teams = [range(s, min(s + 3, streams)) for s in range(0, streams, 3)]
    to_do = list(range(groups))
    ready = 0
    at_step = {}

    def one_rest():
        if to_do:
            rest_pass(refs, to_do.pop(0), first_state, grads, dq, dk, dd)

    def push():
        for t in list(at_step):
            advance(teams[t], at_step[t])
            at_step[t] += 1
            if at_step[t] == bits:
                del at_step[t]

    for t, team in enumerate(teams):
        for s in team:
            while ready <= s // per_stream:
                value_pass(refs, ready, last_grad, dv, grads)
                ready += 1
            fill(s, range(n // 2, n))
            hop(s, 0).start()
        for s in team:
            fill(s, range(n // 2))
        push()
        at_step[t] = 0
    while at_step:
        one_rest()
        push()
    while to_do:
        one_rest()
    total = jnp.sum(out[...] * out[...], axis=1, keepdims=True)
    own_norm[...] = jnp.broadcast_to(total, own_norm.shape)

    def give(d):
        return pltpu.make_async_remote_copy(
            own_norm, got_norm.at[d], send_n.at[d], recv_n.at[d],
            device_id={"tp": lax.rem(side + d, tp)}, device_id_type=MESH,
        )

    for d in range(1, tp):
        give(d).start()
    for step in range(bits):
        for s in range(streams):
            hop(s, step).wait_send()
    for d in range(1, tp):
        give(d).wait()
    full = own_norm[...]
    for d in range(1, tp):
        full = full + got_norm[d]
    norms[...] = full


def on_device(n, tp, block_input, value_weight, queries, key_rows, log_decay, out_grad):
    rows, model = block_input.shape
    heads = log_decay.shape[1]
    groups = queries.shape[1] // STATE
    per_group = heads // groups
    width = per_group * HEAD_DIM
    blocks = rows // SPAN
    decays = log_decay.T.reshape(groups, per_group, rows)
    xt = block_input.T.reshape(n, model // n, rows)

    def by_group(cols):
        return pl.BlockSpec((rows, cols), lambda i: (0, i))

    ld_spec = pl.BlockSpec((1, per_group, rows), lambda i: (i, 0, 0))
    state_spec = pl.BlockSpec((width, STATE), lambda i: (i, 0))
    state_shape = jax.ShapeDtypeStruct((heads * HEAD_DIM, STATE), F32)
    values, fresh, back, logs = pl.pallas_call(
        own_kernel,
        grid=(groups,),
        in_specs=[
            pl.BlockSpec((rows, model), lambda i: (0, 0)),
            pl.BlockSpec((model, width), lambda i: (0, i)),
            by_group(STATE), by_group(STATE), ld_spec, by_group(width),
        ],
        out_specs=[
            by_group(width), state_spec, state_spec,
            pl.BlockSpec((per_group, 8, LANES), lambda i: (i, 0, 0)),
        ],
        out_shape=[
            jax.ShapeDtypeStruct((rows, heads * HEAD_DIM), BF16), state_shape, state_shape,
            jax.ShapeDtypeStruct((heads, 8, LANES), F32),
        ],
        compiler_params=pltpu.CompilerParams(vmem_limit_bytes=GRANT),
        name="own_states",
    )(block_input, value_weight, queries, key_rows, decays, out_grad)

    vm = pl.BlockSpec(memory_space=VMEM)
    inner = 1 << (bits_of(n) // 2)
    outer = n // inner
    chunk = heads * HEAD_DIM // inner
    tall = max(1, chunk // HEAD_DIM)
    own = (tall, chunk // tall, STATE)
    piece = (inner, *own)
    log = (tall, 8, LANES)
    dma = pltpu.SemaphoreType.DMA
    before, after = pl.pallas_call(
        functools.partial(scan_kernel, inner, outer),
        in_specs=[vm] * 3,
        out_specs=[vm] * 2,
        out_shape=[jax.ShapeDtypeStruct(piece, F32)] * 2,
        scratch_shapes=[VMEM(piece, F32)] * 2 + [VMEM((inner, *log), F32)] + [VMEM(piece, F32)] * 2
        + [VMEM((2, *own), F32), VMEM(log, F32), VMEM((outer, *own), F32), VMEM((outer, *log), F32)]
        + [dma((3, inner))] * 2 + [dma((2, outer))] * 2 + [dma((2, inner))] * 2,
        compiler_params=pltpu.CompilerParams(collective_id=0, has_side_effects=True, vmem_limit_bytes=GRANT),
        name="scan_states",
    )(fresh.reshape(piece), back.reshape(piece), logs)

    own_rows, columns = model // n, heads * HEAD_DIM
    streams = columns // LANES
    bits = bits_of(n)
    query_grad, key_grad, decay_rows, weight_grad, norms = pl.pallas_call(
        functools.partial(weight_kernel, n, tp),
        in_specs=[vm] * 8,
        out_specs=[vm] * 5,
        out_shape=[
            jax.ShapeDtypeStruct(queries.shape, F32), jax.ShapeDtypeStruct(queries.shape, F32),
            jax.ShapeDtypeStruct((groups, per_group, rows), F32),
            jax.ShapeDtypeStruct((own_rows, columns), F32),
            jax.ShapeDtypeStruct((own_rows, LANES), F32),
        ],
        scratch_shapes=[
            VMEM((streams, n, own_rows, LANES), F32), VMEM((rows, columns), BF16),
            VMEM((groups, blocks, width, STATE), F32),
            VMEM((own_rows, LANES), F32), VMEM((tp, own_rows, LANES), F32),
        ]
        + [VMEM((streams, n >> (b + 1), own_rows, LANES), F32) for b in range(bits)]
        + [pltpu.SemaphoreType.DMA((streams, bits))] * 2 + [pltpu.SemaphoreType.DMA((tp,))] * 2,
        compiler_params=pltpu.CompilerParams(collective_id=1, has_side_effects=True, vmem_limit_bytes=GRANT),
        name="weight_grad",
    )(xt, queries, key_rows, values, out_grad, decays,
      before.reshape(heads * HEAD_DIM, STATE), after.reshape(heads * HEAD_DIM, STATE))
    return query_grad, key_grad, decay_rows.reshape(heads, rows).T, weight_grad, norms[:, 0]


def solution(mesh):
    in_specs = (
        P("sp", None),
        P(None, "tp"),
        P("sp", "tp"),
        P("sp", "tp"),
        P("sp", "tp"),
        P("sp", "tp"),
    )
    out_specs = (P("sp", "tp"), P("sp", "tp"), P("sp", "tp"), P("sp", "tp"), P("sp"))
    return jax.shard_map(
        functools.partial(on_device, mesh.shape["sp"], mesh.shape["tp"]),
        mesh=mesh, in_specs=in_specs, out_specs=out_specs, check_vma=False,
    )
```
